32 devices in a mesh: sp: 8 (over z, y), dp: 4 (over x, core).
Axes of the slice: x: 2, y: 2, z: 4, core: 2. Of those that a mesh axis runs over, the one named last changes fastest.
Arguments:
- tokens: bfloat16 [4, 4096, 2048], P('dp', 'sp'), may hold values from -6 to 6
- norm_gain: float32 [2048], replicated, may hold values from 0.1 to 1.9
- w_query: bfloat16 [2048, 1024], P(('sp', 'dp')), may hold values from -0.125 to 0.125
- w_key: bfloat16 [2048, 1024], P(('sp', 'dp')), may hold values from -0.125 to 0.125
- w_value: bfloat16 [2048, 2048], P(('sp', 'dp')), may hold values from -0.125 to 0.125
- w_out: bfloat16 [2048, 2048], P(('sp', 'dp')), may hold values from -0.125 to 0.125
- decay_rate: float32 [4, 8, 32], P('dp'), may hold values from 1.2207031e-05 to 0.08, as said below
Outputs:
- layer_out: bfloat16 [4, 4096, 2048], P('dp', 'sp')
The draws below stay inside these ranges and needn't reach their ends.
Inputs may be any that keep to these rules, and one draw needn't show every extreme that they name: `decay_rate`: one rate for each sequence, head and block of 128 positions.
All inputs are finite; a program needn't handle non-finite values.
Results may differ from the reference program's by a relative error of at most 0.02.
Values may be sent and summed in bfloat16 or wider, within the bound.
A program may use at most 128 MiB of HBM per device.

```python
import jax
import jax.numpy as jnp
from jax import lax

D = 2048
HEADS = 8
DK = 128
DV = 256
GROUP_W = 128
BLOCK = 128
SEQ = 4096
BATCH = 4


def draw_decay_rate(key, part):
    subkeys = jax.random.split(jax.random.fold_in(key, 17), 4)
    block_count = SEQ // BLOCK
    ranking = jax.vmap(lambda single: jax.random.permutation(single, HEADS))(jax.random.split(subkeys[0], BATCH))
    fast_count = HEADS // 2
    is_fast = ranking < fast_count
    slow_base = jnp.exp(jax.random.uniform(subkeys[1], (BATCH, HEADS), jnp.float32, jnp.log(0.1), jnp.log(0.5))) / SEQ
    fast_base = jnp.exp(jax.random.uniform(subkeys[2], (BATCH, HEADS), jnp.float32, jnp.log(0.02), jnp.log(0.04)))
    base_rate = jnp.where(is_fast, fast_base, slow_base)
    factor = jnp.exp(jax.random.uniform(subkeys[3], (BATCH, HEADS, block_count), jnp.float32, jnp.log(0.5), jnp.log(2.0)))
    return base_rate[:, :, None] * factor


def level_of(stream_key, dims, cuts, least, top_value):
    gain = 1.0
    for axis_at, blocks in cuts:
        heights = jax.random.uniform(jax.random.fold_in(jax.random.fold_in(stream_key, 6), axis_at), (blocks,), jnp.float32, least / len(cuts), top_value / len(cuts))
        gain = gain * jnp.repeat(jnp.exp(heights), dims[axis_at] // blocks).reshape((-1,) + (1,) * (len(dims) - 1 - axis_at))
    return gain


def gaussian(own_key, dims, scale, reach, cuts=(), kind=jnp.bfloat16):
    values = jax.random.normal(own_key, dims, jnp.float32) * scale
    if len(cuts) > 0:
        values = level_of(own_key, dims, cuts, -0.22, 0.18) * values
    return jnp.clip(values, min=-reach, max=reach).astype(kind)


def setup_inputs(seed: int = 0) -> dict:
    arg_keys = jax.random.split(jax.random.key(seed), 8)
    return {
        "tokens": gaussian(arg_keys[0], (BATCH, SEQ, D), 1.0, 6.0, ((0, 4), (1, 8))),
        "norm_gain": jnp.clip(1.0 + 0.18 * jax.random.normal(arg_keys[1], (D,), jnp.float32), 0.1, 1.9),
        "w_query": gaussian(arg_keys[2], (D, HEADS * DK), D ** -0.5, 0.125, ((0, 32),)),
        "w_key": gaussian(arg_keys[3], (D, HEADS * DK), D ** -0.5, 0.125, ((0, 32),)),
        "w_value": gaussian(arg_keys[4], (D, HEADS * DV), D ** -0.5, 0.125, ((0, 32),)),
        "w_out": gaussian(arg_keys[5], (HEADS * DV, D), (HEADS * DV) ** -0.5, 0.125, ((0, 32),)),
        "decay_rate": draw_decay_rate(jax.random.fold_in(arg_keys[7], 71), 0),
    }


EPS_RMS = 1e-06
EPS_GROUP = 0.01
ROPE_BASE = 10000.0

def rms_scaled(token_rows, norm_gain):
    widened = token_rows.astype(jnp.float32)
    inv_norm = lax.rsqrt(lax.optimization_barrier(jnp.mean(widened * widened, axis=-1, keepdims=True)) + EPS_RMS)
    return (widened * inv_norm * norm_gain).astype(jnp.bfloat16)

def rope_tables(length, head_depth):
    half_depth = head_depth // 2
    inverse = ROPE_BASE ** (-(jnp.arange(half_depth, dtype=jnp.float32) / (half_depth - 1)))
    angles = jnp.arange(length, dtype=jnp.float32)[:, None] * inverse[None, :]
    return (jnp.cos(angles), jnp.sin(angles))

def rotate(stacked, cosine_table, sine_table):
    paired = stacked.reshape(stacked.shape[0], stacked.shape[1], -1, 2)
    first_part = paired[..., 0]
    second_part = paired[..., 1]
    cos_rows = cosine_table[:, None, :]
    sin_rows = sine_table[:, None, :]
    turned = jnp.stack([first_part * cos_rows - second_part * sin_rows, second_part * cos_rows + first_part * sin_rows], axis=-1)
    return turned.reshape(stacked.shape)

def rounded_copy(widened):
    return lax.optimization_barrier(widened.astype(jnp.bfloat16)).astype(jnp.float32)

def retain(queries, keys_in, values_in, decay_rows):
    length, groups, head_depth = queries.shape
    channel_width = values_in.shape[-1]
    blocks = length // BLOCK

    def by_block(stacked):
        return stacked.astype(jnp.float32).reshape(blocks, BLOCK, groups, stacked.shape[-1]).transpose(2, 0, 1, 3)
    query_blocks = by_block(queries)
    key_blocks = by_block(keys_in)
    value_blocks = by_block(values_in)
    offsets = jnp.arange(BLOCK, dtype=jnp.float32)
    distance = offsets[:, None] - offsets[None, :]
    within = jnp.where(distance >= 0.0, jnp.exp(-decay_rows[:, :, None, None] * jnp.maximum(distance, 0.0)), 0.0)
    scores = jnp.einsum('gncd,gnmd->gncm', query_blocks, key_blocks)
    weighted = rounded_copy(scores * within)
    inner_sum = jnp.einsum('gncm,gnme->gnce', weighted, value_blocks)
    to_end = jnp.exp(-decay_rows[:, :, None] * (BLOCK - 1.0 - offsets))
    key_scaled = rounded_copy(key_blocks * to_end[..., None])
    local_state = jnp.einsum('gncd,gnce->gnde', key_scaled, value_blocks)
    carried = jnp.exp(-decay_rows * BLOCK)

    def advance(running, inputs):
        decay_now, added = inputs
        return (decay_now[:, None, None] * running + added, running)
    start_state = jnp.zeros((groups, head_depth, channel_width), jnp.float32)
    _, before = lax.scan(advance, start_state, (carried.T, local_state.transpose(1, 0, 2, 3)))
    from_start = jnp.exp(-decay_rows[:, :, None] * (offsets + 1.0))
    cross_term = jnp.einsum('gncd,ngde->gnce', query_blocks * from_start[..., None], before, precision=lax.Precision.HIGHEST)
    mixed = inner_sum + cross_term
    return mixed.transpose(1, 2, 0, 3).reshape(length, groups, channel_width)

def reference(tokens, norm_gain, w_query, w_key, w_value, w_out, decay_rate):

    def per_sequence(inputs):
        token_rows, decay_rows = inputs
        length = token_rows.shape[0]
        normed_in = rms_scaled(token_rows, norm_gain)
        query_proj = jnp.dot(normed_in, w_query, preferred_element_type=jnp.float32).astype(jnp.bfloat16)
        key_proj = jnp.dot(normed_in, w_key, preferred_element_type=jnp.float32).astype(jnp.bfloat16)
        value_proj = jnp.dot(normed_in, w_value, preferred_element_type=jnp.float32).astype(jnp.bfloat16)
        cosine_table, sine_table = rope_tables(length, DK)
        query_rot = rotate(query_proj.astype(jnp.float32).reshape(length, HEADS, DK), cosine_table, sine_table).astype(jnp.bfloat16)
        key_rot = (rotate(key_proj.astype(jnp.float32).reshape(length, HEADS, DK), cosine_table, sine_table) * DK ** (-0.5)).astype(jnp.bfloat16)
        mixed = retain(jnp.concatenate([query_rot, query_rot], axis=1), jnp.concatenate([key_rot, key_rot], axis=1), value_proj.reshape(length, 2 * HEADS, GROUP_W), jnp.concatenate([decay_rows, decay_rows], axis=0))
        halves = mixed.reshape(length, 2, HEADS, GROUP_W)
        mean_part = lax.optimization_barrier(jnp.sum(halves, axis=(1, 3), keepdims=True)) / DV
        square_part = lax.optimization_barrier(jnp.sum(halves * halves, axis=(1, 3), keepdims=True)) / DV
        retained = ((halves - mean_part) * lax.rsqrt(square_part - mean_part * mean_part + EPS_GROUP)).astype(jnp.bfloat16)
        return jnp.dot(retained.reshape(length, 2 * HEADS * GROUP_W), w_out, preferred_element_type=jnp.float32).astype(jnp.bfloat16)
    return lax.map(per_sequence, (tokens, decay_rate))
```

```python
import jax
import jax.numpy as jnp
import functools
from jax import lax
from jax.experimental import pallas as pl
from jax.experimental.pallas import tpu as pltpu
from jax.sharding import PartitionSpec as P

HEADS = 8
DK = 128
DV = 256
GROUP_W = 128
BLOCK = 128


EPS_RMS = 1e-06
EPS_GROUP = 0.01
ROPE_BASE = 10000.0
MESH = pl.DeviceIdType.MESH

LINE_ORDERS = ((0, 1, 2), (0, 2, 1), (1, 2, 0), (2, 1, 0))
SHARE = (3, 3, 1, 1)
WAVES = 3
SKEW = 2


def chip_grid(mesh_shape):
    sp, dp = mesh_shape["sp"], mesh_shape["dp"]
    y_size = max(k for k in range(1, sp + 1) if sp % k == 0 and k * k <= sp)
    return (sp // y_size, y_size, dp // 2)


def project_kernel(grid, x_ref, gain_ref, own_ref, proj_ref, out_w_ref, g_ref, normed_ref,
                   own_sem, out_sem, recv_sem, pair_recv, send_sem, pair_send):
    z_size, y_size, x_size = grid
    chips = z_size * y_size * x_size
    rows = own_ref.shape[0]
    width = own_ref.shape[1] // WAVES
    sp_at = lax.axis_index("sp")
    dp_at = lax.axis_index("dp")
    core = lax.rem(dp_at, 2)
    here = (sp_at // y_size, lax.rem(sp_at, y_size), dp_at // 2)

    def device(place, core_at):
        return {"sp": place[0] * y_size + place[1], "dp": place[2] * 2 + core_at}

    def moved(dim, sign):
        return tuple(at + sign if k == dim else at for k, at in enumerate(here))

    def in_range(dim, sign):
        return here[dim] + 1 < grid[dim] if sign > 0 else here[dim] > 0

    ways = [(dim, sign) for dim in range(3) if grid[dim] > 1 for sign in (1, -1)]
    barrier = pltpu.get_barrier_semaphore()
    pl.semaphore_signal(barrier, inc=1, device_id=device(here, 1 - core), device_id_type=MESH)
    peers = 1
    for dim, sign in ways:
        @pl.when(in_range(dim, sign))
        def _(dim=dim, sign=sign):
            pl.semaphore_signal(
                barrier, inc=1, device_id=device(moved(dim, sign), core), device_id_type=MESH
            )
    for dim, sign in ways:
        peers = peers + jnp.where(in_range(dim, sign), 1, 0)
    pl.semaphore_wait(barrier, peers)

    me = (here[0] * y_size + here[1]) * x_size + here[2]

    def row_at(chip, core_at):
        return pl.multiple_of((chip * 2 + core_at) * rows, rows)

    own = pltpu.make_async_copy(own_ref, g_ref.at[pl.ds(row_at(me, core), rows), :], own_sem)
    own.start()
    own.wait()
    unit = width // sum(SHARE)

    def piece(w, q, start, size, core_at):
        first = pl.multiple_of(w * width + start, 128)
        return g_ref.at[pl.ds(row_at(q, core_at), rows), pl.ds(first, size)]

    def copies(w, q):
        found = []
        gone = (
            here[0] - q // (y_size * x_size),
            here[1] - lax.rem(q // x_size, y_size),
            here[2] - lax.rem(q, x_size),
        )
        pair = pltpu.make_async_remote_copy(
            src_ref=piece(w, q, 0, width, core), dst_ref=piece(w, q, 0, width, core),
            send_sem=pair_send.at[q], recv_sem=pair_recv.at[w, q],
            device_id=device(here, 1 - core), device_id_type=MESH,
        )
        start = 0
        for kind, order in enumerate(LINE_ORDERS):
            size = SHARE[kind] * unit
            for spot, (dim, sign) in enumerate(ways):
                keep = in_range(dim, sign) & (gone[dim] * sign >= 0)
                for later in order[order.index(dim) + 1:]:
                    keep = keep & (gone[later] == 0)
                ref = piece(w, q, start, size, core)
                found.append((keep, pltpu.make_async_remote_copy(
                    src_ref=ref, dst_ref=ref,
                    send_sem=send_sem.at[q, kind * len(ways) + spot],
                    recv_sem=recv_sem.at[w, q],
                    device_id=device(moved(dim, sign), core), device_id_type=MESH,
                )))
            start += size
        distance = abs(gone[0]) + abs(gone[1]) + abs(gone[2])
        return distance, pair, found

    def forward(w, r):
        def one(q, _):
            distance, pair, found = copies(w, q)

            @pl.when(distance == r)
            def _():
                @pl.when(r > 0)
                def _():
                    full = piece(w, q, 0, width, core)
                    pltpu.make_async_copy(full, full, recv_sem.at[w, q]).wait()
                for keep, copy in found:
                    @pl.when(keep)
                    def _(copy=copy):
                        copy.start()
                pair.start()
            return 0
        lax.fori_loop(0, chips, one, 0)

    def run(first, last):
        def at(t, _):
            def wave(w, _):
                forward(w, t - SKEW * w)
                return 0
            return lax.fori_loop(0, WAVES, wave, 0)
        lax.fori_loop(first, last, at, 0)

    def pair_done(w):
        def one(q, _):
            full = piece(w, q, 0, width, 1 - core)
            pltpu.make_async_copy(full, full, pair_recv.at[w, q]).wait()
            return 0
        lax.fori_loop(0, chips, one, 0)

    count = x_ref.shape[0]
    tile = 256

    def project(w):
        def one(n, _):
            columns = pl.ds(pl.multiple_of(w * width + n * tile, tile), tile)
            proj_ref[:, columns] = jnp.dot(
                normed_ref[...], g_ref[:, columns], preferred_element_type=jnp.float32
            ).astype(jnp.bfloat16)
            return 0
        lax.fori_loop(0, width // tile, one, 0)

    last_round = sum(size - 1 for size in grid)
    run(0, 1)

    def norm(n, _):
        at = pl.ds(pl.multiple_of(n * 64, 64), 64)
        wide = x_ref[at, :].astype(jnp.float32)
        scale = lax.rsqrt(jnp.mean(wide * wide, axis=-1, keepdims=True) + EPS_RMS)
        normed_ref[at, :] = (wide * scale * gain_ref[...]).astype(jnp.bfloat16)
        return 0
    lax.fori_loop(0, count // 64, norm, 0)

    run(1, last_round + 1)
    pair_done(0)
    project(0)
    run(last_round + 1, last_round + SKEW + 1)
    pair_done(1)
    project(1)
    run(last_round + SKEW + 1, last_round + 2 * SKEW + 1)
    pair_done(2)
    leave = pltpu.make_async_copy(g_ref.at[:, pl.ds(2 * width, width)], out_w_ref, out_sem)
    leave.start()

    def drain(q, _):
        _, _, found = copies(0, q)
        for slot, (keep, _) in enumerate(found):
            @pl.when(keep)
            def _(slot=slot):
                sent = piece(0, q, 0, WAVES * SHARE[slot // len(ways)] * unit, core)
                pltpu.make_async_copy(sent, sent, send_sem.at[q, slot]).wait()
        sent = piece(0, q, 0, WAVES * width, core)
        pltpu.make_async_copy(sent, sent, pair_send.at[q]).wait()
        return 0
    lax.fori_loop(0, chips, drain, 0)
    leave.wait()


def projected(grid, token_rows, norm_gain, own_rows):
    count, depth = token_rows.shape
    rows, columns = own_rows.shape
    width = columns // WAVES
    chips = grid[0] * grid[1] * grid[2]
    ways = 2 * sum(size > 1 for size in grid)
    vmem = pl.BlockSpec(memory_space=pltpu.VMEM)
    hbm = pl.BlockSpec(memory_space=pl.ANY)
    return pl.pallas_call(
        functools.partial(project_kernel, grid),
        out_shape=(
            jax.ShapeDtypeStruct((count, 2 * width), jnp.bfloat16),
            jax.ShapeDtypeStruct((depth, width), jnp.bfloat16),
        ),
        in_specs=[vmem, vmem, hbm],
        out_specs=(vmem, hbm),
        scratch_shapes=[
            pltpu.VMEM((depth, columns), jnp.bfloat16),
            pltpu.VMEM((count, depth), jnp.bfloat16),
            pltpu.SemaphoreType.DMA,
            pltpu.SemaphoreType.DMA,
            pltpu.SemaphoreType.DMA((WAVES, chips)),
            pltpu.SemaphoreType.DMA((WAVES, chips)),
            pltpu.SemaphoreType.DMA((chips, 4 * ways)),
            pltpu.SemaphoreType.DMA((chips,)),
        ],
        compiler_params=pltpu.CompilerParams(
            collective_id=0, has_side_effects=True, vmem_limit_bytes=60 * 1024 * 1024
        ),
    )(token_rows, norm_gain[None, :], own_rows)


def carried_in(x, axis, join, neutral):
    place = lax.axis_index(axis)
    gathered = jax.tree.map(
        lambda a, kind: lax.all_gather(a.astype(kind), axis), x, (jnp.bfloat16, jnp.bfloat16)
    )
    state = jax.tree.map(lambda a, e: jnp.zeros_like(a) + jnp.asarray(e, a.dtype), x, neutral)

    def one(lap, state):
        return join(
            state,
            jax.tree.map(
                lambda a, own: lax.dynamic_index_in_dim(a, lap, 0, False).astype(own.dtype),
                gathered,
                x,
            ),
        )

    return lax.fori_loop(0, place, one, state)


def rope_tables(length, head_depth, first_pos):
    half_depth = head_depth // 2
    inverse = ROPE_BASE ** (-(jnp.arange(half_depth, dtype=jnp.float32) / (half_depth - 1)))
    places = first_pos.astype(jnp.float32) + jnp.arange(length, dtype=jnp.float32)
    angles = places[:, None] * inverse[None, :]
    return (jnp.cos(angles), jnp.sin(angles))


def rotate(stacked, cosine_table, sine_table):
    paired = stacked.reshape(stacked.shape[0], stacked.shape[1], -1, 2)
    first_part = paired[..., 0]
    second_part = paired[..., 1]
    cos_rows = cosine_table[:, None, :]
    sin_rows = sine_table[:, None, :]
    turned = jnp.stack(
        [
            first_part * cos_rows - second_part * sin_rows,
            second_part * cos_rows + first_part * sin_rows,
        ],
        axis=-1,
    )
    return turned.reshape(stacked.shape)


def combine_pairs(earlier, later):
    return (earlier[0] * later[0], later[0][..., None, None] * earlier[1] + later[1])


def from_earlier(last_decay, last_state):
    _, incoming = carried_in(
        (last_decay, last_state),
        "sp",
        combine_pairs,
        (jnp.ones_like(last_decay), jnp.zeros_like(last_state)),
    )
    return incoming


def retain(queries, keys_in, values_in, decay_rows, carry_in):
    length, groups, head_depth = queries.shape
    blocks = length // BLOCK

    def by_block(stacked):
        return stacked.reshape(blocks, BLOCK, groups, stacked.shape[-1]).transpose(2, 0, 1, 3)

    query_blocks = by_block(queries)
    key_blocks = by_block(keys_in)
    value_blocks = by_block(values_in)
    offsets = jnp.arange(BLOCK, dtype=jnp.float32)
    distance = offsets[:, None] - offsets[None, :]
    within = jnp.where(
        distance >= 0.0, jnp.exp(-decay_rows[:, :, None, None] * jnp.maximum(distance, 0.0)), 0.0
    )
    scores = jnp.einsum(
        "gncd,gnmd->gncm", query_blocks, key_blocks, preferred_element_type=jnp.float32
    )
    weighted = (scores * within).astype(jnp.bfloat16)
    inner_sum = jnp.einsum(
        "gncm,gnme->gnce", weighted, value_blocks, preferred_element_type=jnp.float32
    )
    to_end = jnp.exp(-decay_rows[:, :, None] * (BLOCK - 1.0 - offsets))
    key_scaled = (key_blocks.astype(jnp.float32) * to_end[..., None]).astype(jnp.bfloat16)
    local_state = jnp.einsum(
        "gncd,gnce->gnde", key_scaled, value_blocks, preferred_element_type=jnp.float32
    )
    carried = jnp.exp(-decay_rows * BLOCK)
    cum_decay, cum_state = lax.associative_scan(combine_pairs, (carried, local_state), axis=1)
    incoming = carry_in(cum_decay[:, -1], cum_state[:, -1])
    before_local = jnp.concatenate([jnp.zeros_like(cum_state[:, :1]), cum_state[:, :-1]], axis=1)
    decay_before = jnp.concatenate([jnp.ones_like(cum_decay[:, :1]), cum_decay[:, :-1]], axis=1)
    before = before_local + decay_before[..., None, None] * incoming[:, None]
    from_start = jnp.exp(-decay_rows[:, :, None] * (offsets + 1.0))
    cross_term = jnp.einsum(
        "gncd,gnde->gnce",
        query_blocks.astype(jnp.float32) * from_start[..., None],
        before,
        precision=lax.Precision.HIGHEST,
    )
    mixed = inner_sum + cross_term
    return mixed.transpose(1, 2, 0, 3).reshape(length, groups, values_in.shape[-1])


def body(grid, tokens, norm_gain, w_query, w_key, w_value, w_out, decay_rate):
    token_rows = tokens[0]
    local_count = token_rows.shape[0]
    own_rows = jnp.concatenate([w_key, w_value, w_query, w_out], axis=1)
    proj, out_rows = projected(grid, token_rows, norm_gain, own_rows)
    key_end = w_key.shape[1]
    value_end = key_end + w_value.shape[1]
    key_sum = proj[:, :key_end]
    value_sum = proj[:, key_end:value_end]
    query_sum = proj[:, value_end:]
    shard_index = lax.axis_index("sp")
    cosine_table, sine_table = rope_tables(local_count, DK, shard_index * local_count)
    query_rot = rotate(
        query_sum.astype(jnp.bfloat16).astype(jnp.float32).reshape(local_count, HEADS, DK),
        cosine_table,
        sine_table,
    ).astype(jnp.bfloat16)
    key_rot = (
        rotate(
            key_sum.astype(jnp.bfloat16).astype(jnp.float32).reshape(local_count, HEADS, DK),
            cosine_table,
            sine_table,
        )
        * DK ** (-0.5)
    ).astype(jnp.bfloat16)
    value_groups = value_sum.astype(jnp.bfloat16).reshape(local_count, 2 * HEADS, GROUP_W)
    blocks_here = local_count // BLOCK
    own_rates = lax.dynamic_slice_in_dim(decay_rate[0], shard_index * blocks_here, blocks_here, 1)
    mixed = retain(
        jnp.concatenate([query_rot, query_rot], axis=1),
        jnp.concatenate([key_rot, key_rot], axis=1),
        value_groups,
        jnp.concatenate([own_rates, own_rates], axis=0),
        from_earlier,
    )
    halves = mixed.reshape(local_count, 2, HEADS, GROUP_W)
    mean_part = jnp.sum(halves, axis=(1, 3), keepdims=True) / DV
    square_part = jnp.sum(halves * halves, axis=(1, 3), keepdims=True) / DV
    retained = (
        ((halves - mean_part) * lax.rsqrt(square_part - mean_part * mean_part + EPS_GROUP))
        .astype(jnp.bfloat16)
        .reshape(local_count, -1)
    )
    result = jnp.dot(retained, out_rows, preferred_element_type=jnp.float32)
    return result.astype(jnp.bfloat16)[None]


def solution(mesh):
    in_specs = (
        P("dp", "sp", None),
        P(),
        P(("sp", "dp"), None),
        P(("sp", "dp"), None),
        P(("sp", "dp"), None),
        P(("sp", "dp"), None),
        P("dp", None, None),
    )
    out_specs = P("dp", "sp", None)
    return jax.shard_map(functools.partial(body, chip_grid(mesh.shape)), mesh=mesh, in_specs=in_specs, out_specs=out_specs, check_vma=False)
```

```python
import jax
import jax.numpy as jnp
import functools
from jax import lax
from jax.experimental import pallas as pl
from jax.experimental.pallas import tpu as pltpu
from jax.sharding import PartitionSpec as P

HEADS = 8
DK = 128
DV = 256
GROUP_W = 128
BLOCK = 128


EPS_RMS = 1e-06
EPS_GROUP = 0.01
ROPE_BASE = 10000.0
MESH = pl.DeviceIdType.MESH

LINE_ORDERS = ((0, 1, 2), (0, 2, 1), (1, 2, 0), (2, 1, 0))
SHARE = (3, 3, 1, 1)
WAVES = 3
SKEW = 2


def chip_grid(mesh_shape):
    sp, dp = mesh_shape["sp"], mesh_shape["dp"]
    y_size = max(k for k in range(1, sp + 1) if sp % k == 0 and k * k <= sp)
    return (sp // y_size, y_size, dp // 2)


def project_kernel(grid, x_ref, gain_ref, own_ref, proj_ref, out_w_ref, g_ref, normed_ref,
                   own_sem, out_sem, recv_sem, pair_recv, send_sem, pair_send):
    z_size, y_size, x_size = grid
    chips = z_size * y_size * x_size
    rows = own_ref.shape[0]
    width = own_ref.shape[1] // WAVES
    sp_at = lax.axis_index("sp")
    dp_at = lax.axis_index("dp")
    core = lax.rem(dp_at, 2)
    here = (sp_at // y_size, lax.rem(sp_at, y_size), dp_at // 2)

    def device(place, core_at):
        return {"sp": place[0] * y_size + place[1], "dp": place[2] * 2 + core_at}

    def moved(dim, sign):
        return tuple(at + sign if k == dim else at for k, at in enumerate(here))

    def in_range(dim, sign):
        return here[dim] + 1 < grid[dim] if sign > 0 else here[dim] > 0

    ways = [(dim, sign) for dim in range(3) if grid[dim] > 1 for sign in (1, -1)]
    barrier = pltpu.get_barrier_semaphore()
    pl.semaphore_signal(barrier, inc=1, device_id=device(here, 1 - core), device_id_type=MESH)
    peers = 1
    for dim, sign in ways:
        @pl.when(in_range(dim, sign))
        def _(dim=dim, sign=sign):
            pl.semaphore_signal(
                barrier, inc=1, device_id=device(moved(dim, sign), core), device_id_type=MESH
            )
    for dim, sign in ways:
        peers = peers + jnp.where(in_range(dim, sign), 1, 0)
    pl.semaphore_wait(barrier, peers)

    me = (here[0] * y_size + here[1]) * x_size + here[2]

    def row_at(chip, core_at):
        return pl.multiple_of((chip * 2 + core_at) * rows, rows)

    own = pltpu.make_async_copy(own_ref, g_ref.at[pl.ds(row_at(me, core), rows), :], own_sem)
    own.start()
    own.wait()
    unit = width // sum(SHARE)

    def piece(w, q, start, size, core_at):
        first = pl.multiple_of(w * width + start, 128)
        return g_ref.at[pl.ds(row_at(q, core_at), rows), pl.ds(first, size)]

    def copies(w, q):
        found = []
        gone = (
            here[0] - q // (y_size * x_size),
            here[1] - lax.rem(q // x_size, y_size),
            here[2] - lax.rem(q, x_size),
        )
        pair = pltpu.make_async_remote_copy(
            src_ref=piece(w, q, 0, width, core), dst_ref=piece(w, q, 0, width, core),
            send_sem=pair_send.at[q], recv_sem=pair_recv.at[w, q],
            device_id=device(here, 1 - core), device_id_type=MESH,
        )
        start = 0
        for kind, order in enumerate(LINE_ORDERS):
            size = SHARE[kind] * unit
            for spot, (dim, sign) in enumerate(ways):
                keep = in_range(dim, sign) & (gone[dim] * sign >= 0)
                for later in order[order.index(dim) + 1:]:
                    keep = keep & (gone[later] == 0)
                ref = piece(w, q, start, size, core)
                found.append((keep, pltpu.make_async_remote_copy(
                    src_ref=ref, dst_ref=ref,
                    send_sem=send_sem.at[q, kind * len(ways) + spot],
                    recv_sem=recv_sem.at[w, q],
                    device_id=device(moved(dim, sign), core), device_id_type=MESH,
                )))
            start += size
        distance = abs(gone[0]) + abs(gone[1]) + abs(gone[2])
        return distance, pair, found

    def forward(w, r):
        def one(q, _):
            distance, pair, found = copies(w, q)

            @pl.when(distance == r)
            def _():
                @pl.when(r > 0)
                def _():
                    full = piece(w, q, 0, width, core)
                    pltpu.make_async_copy(full, full, recv_sem.at[w, q]).wait()
                for keep, copy in found:
                    @pl.when(keep)
                    def _(copy=copy):
                        copy.start()
                pair.start()
            return 0
        lax.fori_loop(0, chips, one, 0)

    def run(first, last):
        def at(t, _):
            def wave(w, _):
                forward(w, t - SKEW * w)
                return 0
            return lax.fori_loop(0, WAVES, wave, 0)
        lax.fori_loop(first, last, at, 0)

    def pair_done(w):
        def one(q, _):
            full = piece(w, q, 0, width, 1 - core)
            pltpu.make_async_copy(full, full, pair_recv.at[w, q]).wait()
            return 0
        lax.fori_loop(0, chips, one, 0)

    count = x_ref.shape[0]
    tile = 256

    def project(w):
        def one(n, _):
            columns = pl.ds(pl.multiple_of(w * width + n * tile, tile), tile)
            proj_ref[:, columns] = jnp.dot(
                normed_ref[...], g_ref[:, columns], preferred_element_type=jnp.float32
            ).astype(jnp.bfloat16)
            return 0
        lax.fori_loop(0, width // tile, one, 0)

    last_round = sum(size - 1 for size in grid)
    run(0, 1)

    def norm(n, _):
        at = pl.ds(pl.multiple_of(n * 64, 64), 64)
        wide = x_ref[at, :].astype(jnp.float32)
        scale = lax.rsqrt(jnp.mean(wide * wide, axis=-1, keepdims=True) + EPS_RMS)
        normed_ref[at, :] = (wide * scale * gain_ref[...]).astype(jnp.bfloat16)
        return 0
    lax.fori_loop(0, count // 64, norm, 0)

    run(1, last_round + 1)
    pair_done(0)
    project(0)
    run(last_round + 1, last_round + SKEW + 1)
    pair_done(1)
    project(1)
    run(last_round + SKEW + 1, last_round + 2 * SKEW + 1)
    pair_done(2)
    leave = pltpu.make_async_copy(g_ref.at[:, pl.ds(2 * width, width)], out_w_ref, out_sem)
    leave.start()

    def drain(q, _):
        _, _, found = copies(0, q)
        for slot, (keep, _) in enumerate(found):
            @pl.when(keep)
            def _(slot=slot):
                sent = piece(0, q, 0, WAVES * SHARE[slot // len(ways)] * unit, core)
                pltpu.make_async_copy(sent, sent, send_sem.at[q, slot]).wait()
        sent = piece(0, q, 0, WAVES * width, core)
        pltpu.make_async_copy(sent, sent, pair_send.at[q]).wait()
        return 0
    lax.fori_loop(0, chips, drain, 0)
    leave.wait()


def projected(grid, token_rows, norm_gain, own_rows):
    count, depth = token_rows.shape
    rows, columns = own_rows.shape
    width = columns // WAVES
    chips = grid[0] * grid[1] * grid[2]
    ways = 2 * sum(size > 1 for size in grid)
    vmem = pl.BlockSpec(memory_space=pltpu.VMEM)
    hbm = pl.BlockSpec(memory_space=pl.ANY)
    return pl.pallas_call(
        functools.partial(project_kernel, grid),
        out_shape=(
            jax.ShapeDtypeStruct((count, 2 * width), jnp.bfloat16),
            jax.ShapeDtypeStruct((depth, width), jnp.bfloat16),
        ),
        in_specs=[vmem, vmem, hbm],
        out_specs=(vmem, hbm),
        scratch_shapes=[
            pltpu.VMEM((depth, columns), jnp.bfloat16),
            pltpu.VMEM((count, depth), jnp.bfloat16),
            pltpu.SemaphoreType.DMA,
            pltpu.SemaphoreType.DMA,
            pltpu.SemaphoreType.DMA((WAVES, chips)),
            pltpu.SemaphoreType.DMA((WAVES, chips)),
            pltpu.SemaphoreType.DMA((chips, 4 * ways)),
            pltpu.SemaphoreType.DMA((chips,)),
        ],
        compiler_params=pltpu.CompilerParams(
            collective_id=0, has_side_effects=True, vmem_limit_bytes=60 * 1024 * 1024
        ),
    )(token_rows, norm_gain[None, :], own_rows)


def rope_tables(length, head_depth, first_pos):
    half_depth = head_depth // 2
    entry = jnp.arange(head_depth)
    inverse = ROPE_BASE ** (-((entry // 2).astype(jnp.float32) / (half_depth - 1)))
    places = first_pos.astype(jnp.float32) + jnp.arange(length, dtype=jnp.float32)
    angles = places[:, None] * inverse[None, :]
    sign = jnp.where(entry % 2 == 0, -1.0, 1.0)
    return (jnp.cos(angles), jnp.sin(angles) * sign)


def retain_kernel(shards, proj_ref, cos_ref, sin_ref, rate_ref, kept_ref, key_ref, query_ref,
                  before_ref, local_ref, inner_ref, sent_ref, came_ref, send_sem, recv_sem):
    place = lax.axis_index("sp")
    dp_at = lax.axis_index("dp")
    count = proj_ref.shape[0]
    blocks = count // BLOCK
    value_at = HEADS * DK
    half = HEADS * GROUP_W
    query_at = value_at + 2 * half
    first, last = place == 0, place == shards - 1

    barrier = pltpu.get_barrier_semaphore()

    @pl.when(jnp.logical_not(first))
    def _():
        pl.semaphore_signal(
            barrier, inc=1, device_id={"sp": place - 1, "dp": dp_at}, device_id_type=MESH
        )

    @pl.when(jnp.logical_not(last))
    def _():
        pl.semaphore_signal(
            barrier, inc=1, device_id={"sp": place + 1, "dp": dp_at}, device_id_type=MESH
        )

    pl.semaphore_wait(barrier, jnp.where(first, 0, 1) + jnp.where(last, 0, 1))

    def columns(start, h):
        return pl.ds(pl.multiple_of(start + h * DK, DK), DK)

    def turned(start, h, n):
        rows = pl.ds(n * BLOCK, BLOCK)
        own = proj_ref[rows, columns(start, h)].astype(jnp.float32)
        even = lax.rem(lax.broadcasted_iota(jnp.int32, own.shape, 1), 2) == 0
        other = jnp.where(even, pltpu.roll(own, DK - 1, 1), pltpu.roll(own, 1, 1))
        return own * cos_ref[rows, :] + other * sin_ref[rows, :]

    def values(h, n):
        rows = pl.ds(n * BLOCK, BLOCK)
        return jnp.concatenate(
            [proj_ref[rows, columns(value_at, h)], proj_ref[rows, columns(value_at + half, h)]],
            axis=1,
        )

    def fade(total):
        return jnp.exp(jnp.full((1, DV), -total * BLOCK, jnp.float32))

    def hand_on(h):
        return pltpu.make_async_remote_copy(
            src_ref=sent_ref.at[h], dst_ref=came_ref.at[h],
            send_sem=send_sem.at[h], recv_sem=recv_sem.at[h],
            device_id={"sp": place + 1, "dp": dp_at}, device_id_type=MESH,
        )

    def local_part(h, _):
        state = jnp.zeros((DK, DV), jnp.float32)
        offset = lax.broadcasted_iota(jnp.int32, (BLOCK, DK), 0).astype(jnp.float32)
        for n in range(blocks):
            rate = rate_ref[h, n]
            key_rot = (turned(0, h, n) * DK ** (-0.5)).astype(jnp.bfloat16)
            key_ref[h, n] = key_rot
            scaled = (
                key_rot.astype(jnp.float32) * jnp.exp(-rate * (BLOCK - 1.0 - offset))
            ).astype(jnp.bfloat16)
            before_ref[h, n] = state
            state = fade(rate) * state + lax.dot_general(
                scaled, values(h, n), (((0,), (0,)), ((), ())),
                preferred_element_type=jnp.float32,
            )
        local_ref[h] = state

        @pl.when(first)
        def _():
            came_ref[h] = jnp.zeros((DK, DV), jnp.bfloat16)
            sent_ref[h] = state.astype(jnp.bfloat16)
            hand_on(h).start()
        return 0

    def inner_part(h, _):
        shape = (BLOCK, BLOCK)
        distance = (
            lax.broadcasted_iota(jnp.int32, shape, 0) - lax.broadcasted_iota(jnp.int32, shape, 1)
        ).astype(jnp.float32)
        for n in range(blocks):
            query_rot = turned(query_at, h, n).astype(jnp.bfloat16)
            query_ref[h, n] = query_rot
            scores = lax.dot_general(
                query_rot, key_ref[h, n], (((1,), (1,)), ((), ())),
                preferred_element_type=jnp.float32,
            )
            within = jnp.where(
                distance >= 0.0, jnp.exp(-rate_ref[h, n] * jnp.maximum(distance, 0.0)), 0.0
            )
            inner_ref[h, n] = jnp.dot(
                (scores * within).astype(jnp.bfloat16), values(h, n),
                preferred_element_type=jnp.float32,
            )
        return 0

    def chain_part(h, _):
        total = rate_ref[h, 0]
        for n in range(1, blocks):
            total = total + rate_ref[h, n]
        pltpu.make_async_copy(came_ref.at[h], came_ref.at[h], recv_sem.at[h]).wait()

        @pl.when(jnp.logical_not(last))
        def _():
            sent_ref[h] = (
                fade(total) * came_ref[h].astype(jnp.float32) + local_ref[h]
            ).astype(jnp.bfloat16)
            hand_on(h).start()
        return 0

    def finish_part(h, _):
        incoming = came_ref[h].astype(jnp.float32)
        offset = lax.broadcasted_iota(jnp.int32, (BLOCK, DV), 0).astype(jnp.float32)
        total = jnp.float32(0.0)
        for n in range(blocks):
            rate = rate_ref[h, n]
            before = before_ref[h, n] + fade(total) * incoming
            cross = jnp.dot(
                query_ref[h, n], before.astype(jnp.bfloat16), preferred_element_type=jnp.float32
            )
            mixed = inner_ref[h, n] + jnp.exp(-rate * (offset + 1.0)) * cross
            mean = jnp.sum(mixed, axis=1, keepdims=True) / DV
            square = jnp.sum(mixed * mixed, axis=1, keepdims=True) / DV
            kept = (
                (mixed - mean) * lax.rsqrt(square - mean * mean + EPS_GROUP)
            ).astype(jnp.bfloat16)
            rows = pl.ds(n * BLOCK, BLOCK)
            kept_ref[rows, columns(0, h)] = kept[:, :GROUP_W]
            kept_ref[rows, columns(half, h)] = kept[:, GROUP_W:]
            total = total + rate
        return 0

    lax.fori_loop(0, HEADS, local_part, 0)
    early = place < shards // 2

    @pl.when(jnp.logical_not(early))
    def _():
        lax.fori_loop(0, HEADS, inner_part, 0)

    @pl.when(jnp.logical_not(first))
    def _():
        lax.fori_loop(0, HEADS, chain_part, 0)

    @pl.when(early)
    def _():
        lax.fori_loop(0, HEADS, inner_part, 0)

    lax.fori_loop(0, HEADS, finish_part, 0)

    @pl.when(jnp.logical_not(last))
    def _():
        def drain(h, _):
            hand_on(h).wait_send()
            return 0
        lax.fori_loop(0, HEADS, drain, 0)


def retained_rows(shards, proj, cosine, sine, own_rates):
    count = proj.shape[0]
    blocks = count // BLOCK
    vmem = pl.BlockSpec(memory_space=pltpu.VMEM)
    return pl.pallas_call(
        functools.partial(retain_kernel, shards),
        out_shape=jax.ShapeDtypeStruct((count, HEADS * DV), jnp.bfloat16),
        in_specs=[vmem, vmem, vmem, pl.BlockSpec(memory_space=pltpu.SMEM)],
        out_specs=vmem,
        scratch_shapes=[
            pltpu.VMEM((HEADS, blocks, BLOCK, DK), jnp.bfloat16),
            pltpu.VMEM((HEADS, blocks, BLOCK, DK), jnp.bfloat16),
            pltpu.VMEM((HEADS, blocks, DK, DV), jnp.float32),
            pltpu.VMEM((HEADS, DK, DV), jnp.float32),
            pltpu.VMEM((HEADS, blocks, BLOCK, DV), jnp.float32),
            pltpu.VMEM((HEADS, DK, DV), jnp.bfloat16),
            pltpu.VMEM((HEADS, DK, DV), jnp.bfloat16),
            pltpu.SemaphoreType.DMA((HEADS,)),
            pltpu.SemaphoreType.DMA((HEADS,)),
        ],
        compiler_params=pltpu.CompilerParams(
            collective_id=1, has_side_effects=True, vmem_limit_bytes=40 * 1024 * 1024
        ),
    )(proj, cosine, sine, own_rates)


def body(grid, tokens, norm_gain, w_query, w_key, w_value, w_out, decay_rate):
    token_rows = tokens[0]
    local_count = token_rows.shape[0]
    own_rows = jnp.concatenate([w_key, w_value, w_query, w_out], axis=1)
    proj, out_rows = projected(grid, token_rows, norm_gain, own_rows)
    shard_index = lax.axis_index("sp")
    cosine, sine = rope_tables(local_count, DK, shard_index * local_count)
    blocks_here = local_count // BLOCK
    own_rates = lax.dynamic_slice_in_dim(decay_rate[0], shard_index * blocks_here, blocks_here, 1)
    retained = retained_rows(grid[0] * grid[1], proj, cosine, sine, own_rates)
    result = jnp.dot(retained, out_rows, preferred_element_type=jnp.float32)
    return result.astype(jnp.bfloat16)[None]


def solution(mesh):
    in_specs = (
        P("dp", "sp", None),
        P(),
        P(("sp", "dp"), None),
        P(("sp", "dp"), None),
        P(("sp", "dp"), None),
        P(("sp", "dp"), None),
        P("dp", None, None),
    )
    out_specs = P("dp", "sp", None)
    return jax.shard_map(functools.partial(body, chip_grid(mesh.shape)), mesh=mesh, in_specs=in_specs, out_specs=out_specs, check_vma=False)
```
